32 devices in a mesh: ep: 16 (over z, x, core), tp: 2 (over y).
Axes of the slice: x: 2, y: 2, z: 4, core: 2. Of those that a mesh axis runs over, the one named last changes fastest.
Arguments:
- tokens: bfloat16 [256, 2048], P('ep'), may hold values from -6 to 6
- attn_gain: bfloat16 [2048], replicated, may hold values from 0.099609375 to 1.8984375
- query_weight: bfloat16 [2048, 1024], P('ep', 'tp'), may hold values from -0.125 to 0.125
- key_weight: bfloat16 [2048, 512], P('ep', 'tp'), may hold values from -0.125 to 0.125
- value_weight: bfloat16 [2048, 512], P('ep', 'tp'), may hold values from -0.125 to 0.125
- out_weight: bfloat16 [2048, 1024], P('ep', 'tp'), may hold values from -0.1875 to 0.1875
- head_gain: bfloat16 [1024], P('tp'), may hold values from 0.099609375 to 1.8984375
- past_keys: bfloat16 [256, 1024, 4, 128], P('ep', None, 'tp'), may hold values from -6 to 6
- past_values: bfloat16 [256, 1024, 4, 128], P('ep', None, 'tp'), may hold values from -50 to 50
- break_offset: float32 [256, 8, 1024], P('ep', 'tp'), may hold values from -12.5 to 1
- cache_lengths: int32 [256], P('ep'), may hold values from 1 to 1024, 131072 in all
- ffn_gain: bfloat16 [2048], replicated, may hold values from 0.099609375 to 1.8984375
- router_weight: bfloat16 [2048, 16], replicated, may hold values from -0.25 to 0.25
- expert_routes: int32 [256, 6], P('ep'), may hold values from 0 to 15, all different within a row; in each aligned block of 16 rows (0 to 15, 16 to 31, ...) at most 12 rows name the same one
- expert_gate: bfloat16 [16, 2048, 512], P('ep', None, 'tp'), may hold values from -0.125 to 0.125
- expert_up: bfloat16 [16, 2048, 512], P('ep', None, 'tp'), may hold values from -0.125 to 0.125
- expert_down: bfloat16 [16, 512, 2048], P('ep', 'tp'), may hold values from -0.25 to 0.25
- shared_gate: bfloat16 [2048, 512], P(None, 'tp'), may hold values from -0.125 to 0.125
- shared_up: bfloat16 [2048, 512], P(None, 'tp'), may hold values from -0.125 to 0.125
- shared_down: bfloat16 [512, 2048], P('tp'), may hold values from -0.25 to 0.25
Outputs:
- mixed: bfloat16 [256, 2048], P('ep', 'tp')
- fresh_keys: bfloat16 [256, 512], P('ep', 'tp')
- fresh_values: bfloat16 [256, 512], P('ep', 'tp')
The draws below stay inside these ranges and needn't reach their ends.
Inputs may be any that keep to these rules, and one draw needn't show every extreme that they name: `cache_lengths`: the lengths add up to half of 262144, and some sequence has length 1024. `expert_routes`: each row names 6 different experts. Among the rows of one device no expert is named more than 12 times, and 12 is reached in some device's rows.
All inputs are finite; a program needn't handle non-finite values. No bound on the sum of `cache_lengths` on one device may be relied on, other than what follows from the above.
Results may differ from the reference program's by a relative error of at most 0.0095.
Values may be sent and summed in bfloat16 or wider, within the bound.
A program may use at most 64 MiB of HBM per device.

```python
import math
import jax
import jax.numpy as jnp
import numpy as np
from jax import lax

D = 2048
HQ = 8
KV = 4
HD = 128
EFF = 512
SFF = 512
TOP_K = 6
SEQ_DEV = 16
CACHE_POSITIONS = 1024
BATCH_SEQUENCES = 256
EXPERTS = 16
CAP = 12
N_EP = 16
N_TP = 2


def draw_break_offset(key, part):
    fast_share = 0.5
    quick_heads = jax.random.uniform(jax.random.fold_in(key, 101), (BATCH_SEQUENCES, HQ, 1)) < fast_share
    baseline_level = jnp.where(quick_heads, math.log(0.08), math.log(0.5 / CACHE_POSITIONS))
    slowdown_factor = jax.random.uniform(jax.random.fold_in(key, 102), (BATCH_SEQUENCES, HQ, 1), minval=0.0, maxval=math.log(3.0))
    jitter_amount = 0.7 * jnp.clip(jax.random.normal(jax.random.fold_in(key, 103), (BATCH_SEQUENCES, HQ, CACHE_POSITIONS)), -5.0, 5.0)
    spike_events = jax.random.uniform(jax.random.fold_in(key, 104), (BATCH_SEQUENCES, 1, CACHE_POSITIONS)) < 3.0 / CACHE_POSITIONS
    spike_level = jax.random.uniform(jax.random.fold_in(key, 105), (BATCH_SEQUENCES, 1, CACHE_POSITIONS), minval=-1.4, maxval=0.0)
    return jnp.where(spike_events, spike_level, baseline_level - slowdown_factor + jitter_amount).astype(jnp.float32)


def draw_past_values(key, part):
    values = jnp.clip(jax.random.normal(jax.random.fold_in(key, 201), (BATCH_SEQUENCES, CACHE_POSITIONS, KV, HD)), -5.0, 5.0)
    top_scale = 3.0
    head_ramp = jnp.arange(KV, dtype=jnp.float32) / max(KV - 1, 1)
    scales = top_scale ** head_ramp
    return (values * scales[None, None, :, None]).astype(jnp.bfloat16)


def block_levels(rng, extent, shards, low, high):
    loudness, own = 1.0, jax.random.fold_in(rng, 6)
    for position, shards_of in shards:
        draws = jnp.exp(jax.random.uniform(jax.random.fold_in(own, position), (shards_of,), jnp.float32, low / len(shards), high / len(shards)))
        loudness = loudness * jnp.repeat(draws, extent[position] // shards_of).reshape([-1 if axis == position else 1 for axis in range(len(extent))])
    return loudness


def length_profile(amount, total, limit, slope):
    portions = [(1 << 20) // math.isqrt(rank ** slope) + 1 for rank in range(2, amount + 1)]
    rest, counts = total - limit - (amount - 1), [1] * (amount - 1)
    while rest > 0:
        free = [i for i in range(amount - 1) if counts[i] < limit]
        pool, left = sum([portions[i] for i in free]), rest
        for i in free:
            more = min(limit - counts[i], max(1, left * portions[i] // pool), rest)
            counts[i] = counts[i] + more
            rest = rest - more
    return np.array([limit] + counts)


def ragged_sizes(own_key, count, total, reach, slope):
    if count == 2:
        one = jax.random.randint(own_key, (), max(1, total - reach), min(reach, total - 1) + 1)
        return jnp.stack([one, total - one])
    sizes = jnp.asarray(length_profile(count, total, reach, slope), jnp.int32)
    couples = (count - 1) // 2
    donor, receiver = sizes[1:1 + 2 * couples:2], sizes[2:2 + 2 * couples:2]
    room = jnp.minimum(donor - 1, reach - receiver)
    moved = jax.random.randint(jax.random.fold_in(own_key, 1), (couples,), 0, 1 << 20) % (room + 1)
    sizes = sizes.at[1:1 + 2 * couples:2].set(donor - moved).at[2:2 + 2 * couples:2].set(receiver + moved)
    return sizes[jax.random.permutation(jax.random.fold_in(own_key, 2), count)]


def routed_block(key, own, number, rows, count, top, most, skew):
    ranking = jax.random.permutation(key, count)
    packed, usual = load_shares(count, rows * top, most, skew, True), load_shares(count, rows * top, most, skew, False)
    places = jnp.arange(count)

    def named(tallies, rotation):
        used = int((tallies > 0).sum())
        fixed = max(1, used // 4)
        shifted = fixed + (places - fixed + rotation * (used - fixed)) % max(1, count - fixed)
        return jnp.zeros((count,), jnp.int32).at[ranking[jnp.where(places < fixed, places, shifted)]].set(jnp.asarray(tallies, jnp.int32))

    tallies = jnp.where(number % 4 == 0, named(packed, number // 4), named(usual, number - number // 4 - 1))
    mixed = jax.random.permutation(jax.random.fold_in(own, 3), count)
    source_of, taker = mixed[0:count // 2 * 2:2], mixed[1:count // 2 * 2:2]
    slack = jnp.minimum(tallies[source_of] - 1, most - tallies[taker]) // 2
    slack = jnp.where((source_of == ranking[0]) | (taker == ranking[0]) | (tallies[taker] == 0), 0, jnp.maximum(slack, 0))
    shifted = jax.random.randint(jax.random.fold_in(own, 4), (count // 2,), 0, 1 << 20) % (slack + 1)
    tallies = tallies.at[source_of].add(-shifted).at[taker].add(shifted)
    members = jnp.searchsorted(jnp.cumsum(tallies), jnp.arange(rows * top), side="right").astype(jnp.int32)
    grid = members.reshape(top, rows).T
    grid = grid[jax.random.permutation(jax.random.fold_in(own, 1), rows)]
    rotation = jax.random.randint(jax.random.fold_in(own, 2), (rows, 1), 0, top)
    return jnp.take_along_axis(grid, (jnp.arange(top)[None, :] + rotation) % top, axis=1)


def load_shares(number_of, total, bound, lean, full):
    loads = [(1 << 20) // math.isqrt(rank ** lean) + 1 for rank in range(1, number_of + 1)]
    largest = bound if full else min(bound, max(-(-total // number_of), total * loads[0] // sum(loads)))
    least = 1 if total - largest >= number_of - 1 else 0
    given, spare = [largest] + [least] * (number_of - 1), total - largest - least * (number_of - 1)
    while spare > 0:
        free = [i for i in range(1, number_of) if given[i] < largest] or [i for i in range(1, number_of) if given[i] < bound]
        whole, remaining = sum([loads[i] for i in free]), spare
        for i in free:
            addition = min(bound - given[i], max(1, remaining * loads[i] // whole), spare)
            given[i] = given[i] + addition
            spare = spare - addition
    return np.array(given)


def noise(own_key, dims, width, bound, cuts=(), kind=jnp.bfloat16):
    result = jax.random.normal(own_key, dims, jnp.float32) * width
    if len(cuts) > 0:
        result = block_levels(own_key, dims, cuts, -0.22, 0.18) * result
    return jnp.clip(result, min=-bound, max=bound).astype(kind)


def setup_inputs(seed: int = 0) -> dict:
    arg_keys = jax.random.split(jax.random.key(seed), 21)
    tokens = noise(arg_keys[0], (BATCH_SEQUENCES, D), 1.0, 6.0, ((0, 16),))
    attn_gain = jnp.clip(1.0 + 0.18 * jax.random.normal(arg_keys[1], (D,), jnp.float32), 0.099609375, 1.8984375).astype(jnp.bfloat16)
    query_weight = noise(arg_keys[2], (D, HQ * HD), D ** -0.5, 0.125, ((0, 16), (1, 2)))
    key_weight = noise(arg_keys[3], (D, KV * HD), D ** -0.5, 0.125, ((0, 16), (1, 2)))
    value_weight = noise(arg_keys[4], (D, KV * HD), D ** -0.5, 0.125, ((0, 16), (1, 2)))
    out_weight = noise(arg_keys[5], (D, HQ * HD), (HQ * HD) ** -0.5, 0.1875, ((0, 16), (1, 2)))
    head_gain = jnp.clip(1.0 + 0.18 * jax.random.normal(arg_keys[6], (HQ * HD,), jnp.float32), 0.099609375, 1.8984375).astype(jnp.bfloat16)
    past_keys = noise(arg_keys[7], (BATCH_SEQUENCES, CACHE_POSITIONS, KV, HD), 1.0, 6.0, ((0, 16), (2, 2)))
    past_values = draw_past_values(jax.random.fold_in(arg_keys[20], 71), 0)
    break_offset = draw_break_offset(jax.random.fold_in(arg_keys[20], 71), 0)
    cache_lengths = ragged_sizes(arg_keys[10], BATCH_SEQUENCES, BATCH_SEQUENCES * CACHE_POSITIONS // 2, CACHE_POSITIONS, 2).astype(jnp.int32)
    ffn_gain = jnp.clip(1.0 + 0.18 * jax.random.normal(arg_keys[11], (D,), jnp.float32), 0.099609375, 1.8984375).astype(jnp.bfloat16)
    router_weight = noise(arg_keys[12], (D, EXPERTS), (D // 4) ** -0.5, 0.25)
    expert_routes_keys = jax.random.split(jax.random.fold_in(arg_keys[13], 1), BATCH_SEQUENCES // SEQ_DEV)
    expert_routes_turns = jax.random.permutation(jax.random.fold_in(arg_keys[13], 3), BATCH_SEQUENCES // SEQ_DEV)
    expert_routes = jax.vmap(lambda own, number: routed_block(jax.random.fold_in(arg_keys[13], 2), own, number, SEQ_DEV, EXPERTS, TOP_K, CAP, 2))(expert_routes_keys, expert_routes_turns).reshape((BATCH_SEQUENCES, TOP_K))
    expert_gate = noise(arg_keys[14], (EXPERTS, D, EFF), D ** -0.5, 0.125, ((0, 16), (2, 2)))
    expert_up = noise(arg_keys[15], (EXPERTS, D, EFF), D ** -0.5, 0.125, ((0, 16), (2, 2)))
    expert_down = noise(arg_keys[16], (EXPERTS, EFF, D), EFF ** -0.5, 0.25, ((0, 16), (1, 2)))
    shared_gate = noise(arg_keys[17], (D, SFF), D ** -0.5, 0.125, ((1, 2),))
    shared_up = noise(arg_keys[18], (D, SFF), D ** -0.5, 0.125, ((1, 2),))
    shared_down = noise(arg_keys[19], (SFF, D), SFF ** -0.5, 0.25, ((0, 2),))
    return {"tokens": tokens, "attn_gain": attn_gain, "query_weight": query_weight, "key_weight": key_weight, "value_weight": value_weight, "out_weight": out_weight, "head_gain": head_gain, "past_keys": past_keys, "past_values": past_values, "break_offset": break_offset, "cache_lengths": cache_lengths, "ffn_gain": ffn_gain, "router_weight": router_weight, "expert_routes": expert_routes, "expert_gate": expert_gate, "expert_up": expert_up, "expert_down": expert_down, "shared_gate": shared_gate, "shared_up": shared_up, "shared_down": shared_down}


epsilon = 1e-06
routed_scale = 2.5

def root_norm(values, gain):
    data = values.astype(jnp.float32)
    factor = lax.rsqrt(lax.optimization_barrier(jnp.mean(data * data, axis=-1, keepdims=True)) + epsilon)
    return (data * factor * gain.astype(jnp.float32)).astype(jnp.bfloat16)

def rounded(values):
    return lax.optimization_barrier(values.astype(jnp.bfloat16)).astype(jnp.float32)

def group_sum(left_side, right_side, groups):
    width_part = left_side.shape[1] // groups
    running = jnp.zeros((left_side.shape[0], right_side.shape[1]), jnp.float32)
    for group_index in range(groups):
        piece_left = left_side[:, group_index * width_part:(group_index + 1) * width_part]
        piece_right = right_side[group_index * width_part:(group_index + 1) * width_part]
        running = running + rounded(jnp.dot(piece_left, piece_right, preferred_element_type=jnp.float32))
    return running

def reference(tokens, attn_gain, query_weight, key_weight, value_weight, out_weight, head_gain, past_keys, past_values, break_offset, cache_lengths, ffn_gain, router_weight, expert_routes, expert_gate, expert_up, expert_down, shared_gate, shared_up, shared_down):
    normed = root_norm(tokens, attn_gain)
    queries = jnp.dot(normed, query_weight, preferred_element_type=jnp.float32).astype(jnp.bfloat16)
    fresh_keys = jnp.dot(normed, key_weight, preferred_element_type=jnp.float32).astype(jnp.bfloat16)
    fresh_values = jnp.dot(normed, value_weight, preferred_element_type=jnp.float32).astype(jnp.bfloat16)
    group_size = HQ // KV

    def attend(inputs):
        block_queries, block_keys, block_values, block_offsets, block_lengths = inputs
        grouped = block_queries.astype(jnp.float32).reshape(SEQ_DEV, KV, group_size, HD)
        scores = jnp.einsum('bgrd,blgd->bgrl', grouped, block_keys.astype(jnp.float32))
        logits = scores.reshape(SEQ_DEV, HQ, CACHE_POSITIONS) * HD ** (-0.5) + block_offsets
        places = jnp.arange(CACHE_POSITIONS, dtype=jnp.int32)[None, None, :]
        usable = places < block_lengths[:, None, None]
        keep_log = jnp.where(usable, jax.nn.log_sigmoid(-logits), 0.0)
        after_sum = lax.cumsum(keep_log, axis=2, reverse=True) - keep_log
        sticks = jnp.where(usable, jnp.exp(jax.nn.log_sigmoid(logits) + after_sum), 0.0)
        sticks = rounded(sticks).reshape(SEQ_DEV, KV, group_size, CACHE_POSITIONS)
        outputs = jnp.einsum('bgrl,blgd->bgrd', sticks, block_values.astype(jnp.float32))
        return outputs.reshape(SEQ_DEV, HQ * HD)
    heads_out = lax.map(attend, (queries.reshape(N_EP, SEQ_DEV, HQ * HD), past_keys.reshape(N_EP, SEQ_DEV, CACHE_POSITIONS, KV, HD), past_values.reshape(N_EP, SEQ_DEV, CACHE_POSITIONS, KV, HD), break_offset.reshape(N_EP, SEQ_DEV, HQ, CACHE_POSITIONS), cache_lengths.reshape(N_EP, SEQ_DEV))).reshape(BATCH_SEQUENCES, HQ * HD)
    scaled = (heads_out * head_gain.astype(jnp.float32)).astype(jnp.bfloat16)
    square_sum = lax.optimization_barrier(jnp.sum(heads_out * heads_out, axis=-1))
    head_total = group_sum(scaled, out_weight.T, N_TP)
    attention = head_total * lax.rsqrt(square_sum[:, None] / (HQ * HD) + epsilon)
    residual = (tokens.astype(jnp.float32) + attention).astype(jnp.bfloat16)
    normed_ffn = root_norm(residual, ffn_gain)
    router_prob = jax.nn.sigmoid(jnp.dot(normed_ffn, router_weight, preferred_element_type=jnp.float32))
    picked = jnp.take_along_axis(router_prob, expert_routes, axis=1)
    route_weight = routed_scale * picked / lax.optimization_barrier(jnp.sum(picked, axis=-1, keepdims=True))
    flat_routes = expert_routes.reshape(N_EP, SEQ_DEV * TOP_K)
    flat_hot = (flat_routes[:, :, None] == jnp.arange(EXPERTS, dtype=jnp.int32)[None, None, :]).astype(jnp.int32)
    earlier = jnp.cumsum(flat_hot, axis=1) - flat_hot
    slot_index = lax.optimization_barrier(jnp.sum(earlier * flat_hot, axis=-1)).astype(jnp.int32)
    owner_group = jnp.broadcast_to(jnp.arange(N_EP, dtype=jnp.int32)[:, None], flat_routes.shape)
    pair_row = jnp.broadcast_to((jnp.arange(SEQ_DEV * TOP_K, dtype=jnp.int32) // TOP_K)[None, :], flat_routes.shape)
    row_number = (owner_group * SEQ_DEV + pair_row).astype(jnp.int32)
    row_table = jnp.full((EXPERTS, N_EP, CAP), BATCH_SEQUENCES, jnp.int32).at[flat_routes, owner_group, slot_index].set(row_number)
    padded_rows = jnp.concatenate([normed_ffn, jnp.zeros((1, D), jnp.bfloat16)], axis=0)

    def one_expert(inputs):
        row_ids, gate_matrix, up_matrix, down_matrix = inputs
        chosen_rows = padded_rows[row_ids.reshape(-1)]
        gate_part = jnp.dot(chosen_rows, gate_matrix, preferred_element_type=jnp.float32)
        up_part = jnp.dot(chosen_rows, up_matrix, preferred_element_type=jnp.float32)
        hidden = (jax.nn.silu(gate_part) * up_part).astype(jnp.bfloat16)
        return group_sum(hidden, down_matrix, N_TP).astype(jnp.bfloat16)
    expert_out = lax.map(one_expert, (row_table, expert_gate, expert_up, expert_down))
    taken = expert_out[flat_routes, (owner_group * CAP + slot_index).astype(jnp.int32)]
    taken = taken.reshape(BATCH_SEQUENCES, TOP_K, D).astype(jnp.float32)
    routed = lax.optimization_barrier(jnp.sum(route_weight[:, :, None] * taken, axis=1))
    shared_hidden = (jax.nn.silu(jnp.dot(normed_ffn, shared_gate, preferred_element_type=jnp.float32)) * jnp.dot(normed_ffn, shared_up, preferred_element_type=jnp.float32)).astype(jnp.bfloat16)
    shared_out = group_sum(shared_hidden, shared_down, N_TP)
    mixed = (residual.astype(jnp.float32) + routed + shared_out).astype(jnp.bfloat16)
    return (mixed, fresh_keys, fresh_values)
```

```python
import functools

import jax
import jax.numpy as jnp
from jax import lax
from jax.experimental import pallas as pl
from jax.experimental.pallas import tpu as pltpu
from jax.sharding import PartitionSpec as P

HQ = 8
HD = 128


epsilon = 1e-06
routed_scale = 2.5


def root_norm(values, gain):
    data = values.astype(jnp.float32)
    factor = lax.rsqrt(jnp.mean(data * data, axis=-1, keepdims=True) + epsilon)
    return (data * factor * gain.astype(jnp.float32)).astype(jnp.bfloat16)


def stick_attend(queries, key_cache, value_cache, offsets, lengths):
    seq_count, positions, key_heads, head_size = key_cache.shape
    heads_local = offsets.shape[1]
    group_size = heads_local // key_heads
    grouped = queries.reshape(seq_count, key_heads, group_size, head_size)
    scores = jnp.einsum("bgrd,blgd->bgrl", grouped, key_cache, preferred_element_type=jnp.float32)
    logits = scores.reshape(seq_count, heads_local, positions) * head_size ** (-0.5) + offsets
    places = lax.broadcasted_iota(jnp.int32, (1, 1, positions), 2)
    usable = places < lengths[:, None, None]
    keep_log = jnp.where(usable, jax.nn.log_sigmoid(-logits), 0.0)
    after_sum = jnp.sum(keep_log, axis=-1, keepdims=True) - jnp.cumsum(keep_log, axis=-1)
    sticks = jnp.where(usable, jnp.exp(jax.nn.log_sigmoid(logits) + after_sum), 0.0).astype(
        jnp.bfloat16
    )
    sticks = sticks.reshape(seq_count, key_heads, group_size, positions)
    outputs = jnp.einsum("bgrl,blgd->bgrd", sticks, value_cache, preferred_element_type=jnp.float32)
    return outputs.reshape(seq_count, heads_local * head_size)


def body(
    tokens,
    attn_gain,
    query_weight,
    key_weight,
    value_weight,
    out_weight,
    head_gain,
    past_keys,
    past_values,
    break_offset,
    cache_lengths,
    ffn_gain,
    router_weight,
    expert_routes,
    expert_gate,
    expert_up,
    expert_down,
    shared_gate,
    shared_up,
    shared_down,
):
    seq_count = tokens.shape[0]
    model_width = tokens.shape[1]
    query_cols = query_weight.shape[1]
    key_cols = key_weight.shape[1]
    normed = root_norm(tokens, attn_gain)
    features = lax.all_to_all(normed, "ep", split_axis=1, concat_axis=0, tiled=True)
    joined = jnp.concatenate([query_weight, key_weight, value_weight], axis=1)
    projected = lax.psum_scatter(
        jnp.dot(features, joined, preferred_element_type=jnp.float32),
        "ep",
        scatter_dimension=0,
        tiled=True,
    )
    queries = projected[:, :query_cols].astype(jnp.bfloat16)
    fresh_keys = projected[:, query_cols : query_cols + key_cols].astype(jnp.bfloat16)
    fresh_values = projected[:, query_cols + key_cols :].astype(jnp.bfloat16)
    experts = router_weight.shape[1]
    top_count = expert_routes.shape[1]
    capacity = max(2, min(seq_count, (2 * seq_count * top_count + experts - 1) // experts))
    local_experts = expert_gate.shape[0]
    column_width = model_width // lax.axis_size("tp")
    block_count = 1
    block_rows = seq_count // block_count
    heads_out = stick_attend(queries, past_keys, past_values, break_offset, cache_lengths)
    scaled = (heads_out * head_gain.astype(jnp.float32)).astype(jnp.bfloat16)
    square_sum = jnp.sum(heads_out * heads_out, axis=-1)
    feature_cols = jnp.einsum(
        "nc,dc->nd",
        lax.all_gather(scaled, "ep", axis=0, tiled=True),
        out_weight,
        preferred_element_type=jnp.float32,
    ).astype(jnp.bfloat16)
    partial_value = lax.all_to_all(feature_cols, "ep", split_axis=0, concat_axis=1, tiled=True)
    all_parts = lax.all_gather(partial_value[None], "tp", axis=0, tiled=True)
    head_total = jnp.sum(all_parts.astype(jnp.float32), axis=0)
    square_total = lax.psum(square_sum, "tp")
    attention = head_total * lax.rsqrt(square_total[:, None] / (HQ * HD) + epsilon)
    residual = (tokens.astype(jnp.float32) + attention).astype(jnp.bfloat16)
    normed_ffn = root_norm(residual, ffn_gain)
    router_prob = jax.nn.sigmoid(
        jnp.dot(normed_ffn, router_weight, preferred_element_type=jnp.float32)
    )
    chosen = expert_routes[:, :, None] == lax.broadcasted_iota(jnp.int32, (1, 1, experts), 2)
    picked = jnp.sum(jnp.where(chosen, router_prob[:, None, :], 0.0), axis=-1)
    route_weight = routed_scale * picked / jnp.sum(picked, axis=-1, keepdims=True)
    flat_hot = chosen.reshape(block_rows * top_count, experts).astype(jnp.int32)
    earlier = jnp.cumsum(flat_hot, axis=0) - flat_hot
    slot_index = jnp.sum(earlier * flat_hot, axis=-1).reshape(block_rows, top_count)
    slot_hot = (
        slot_index[:, :, None] == lax.broadcasted_iota(jnp.int32, (1, 1, capacity), 2)
    ).astype(jnp.float32)
    expert_hot = chosen.astype(jnp.float32)
    dispatch = jnp.einsum("ske,skc->ecs", expert_hot, slot_hot)
    weighted = jnp.sum(
        route_weight[:, :, None, None] * expert_hot[:, :, :, None] * slot_hot[:, :, None, :], axis=1
    )
    outbound = jnp.einsum(
        "ecs,sd->ecd", dispatch.astype(jnp.bfloat16), normed_ffn, preferred_element_type=jnp.float32
    ).astype(jnp.bfloat16)
    arrived = lax.all_to_all(outbound, "ep", split_axis=0, concat_axis=0, tiled=True)
    item_count = arrived.shape[1]
    sources = arrived.shape[0] // local_experts
    grouped = arrived.reshape(sources, local_experts, item_count, model_width)
    gate_part = jnp.einsum(
        "sxcd,xdf->sxcf", grouped, expert_gate, preferred_element_type=jnp.float32
    )
    up_part = jnp.einsum("sxcd,xdf->sxcf", grouped, expert_up, preferred_element_type=jnp.float32)
    hidden = (jax.nn.silu(gate_part) * up_part).astype(jnp.bfloat16)
    down_part = jnp.einsum(
        "sxcf,xfd->sxcd", hidden, expert_down, preferred_element_type=jnp.float32
    )
    expert_part = down_part.astype(jnp.bfloat16).reshape(arrived.shape)
    shared_hidden = (
        jax.nn.silu(jnp.dot(normed_ffn, shared_gate, preferred_element_type=jnp.float32))
        * jnp.dot(normed_ffn, shared_up, preferred_element_type=jnp.float32)
    ).astype(jnp.bfloat16)
    shared_part = jnp.dot(shared_hidden, shared_down, preferred_element_type=jnp.float32).astype(
        jnp.bfloat16
    )
    expert_pieces = lax.all_to_all(expert_part[None], "tp", split_axis=3, concat_axis=0, tiled=True)
    shared_pieces = lax.all_to_all(
        shared_part[None, None], "tp", split_axis=3, concat_axis=0, tiled=True
    )
    expert_total = jnp.sum(expert_pieces.astype(jnp.float32), axis=0)
    shared_total = jnp.sum(shared_pieces.astype(jnp.float32), axis=0)
    returned = lax.all_to_all(
        expert_total.astype(jnp.bfloat16), "ep", split_axis=0, concat_axis=0, tiled=True
    )
    routed = jnp.einsum(
        "sec,ecd->sd", weighted, returned.astype(jnp.float32), precision=lax.Precision.HIGHEST
    )
    own_cols = lax.dynamic_slice_in_dim(
        residual, lax.axis_index("tp") * column_width, column_width, 1
    )
    results = (own_cols.astype(jnp.float32) + routed + shared_total[0]).astype(jnp.bfloat16)
    return (results, fresh_keys, fresh_values)


MESH = pl.DeviceIdType.MESH
F32 = jnp.float32
BF16 = jnp.bfloat16


def fits(ep_count, tp_count, arrays):
    tokens, query_weight, past_keys, break_offset = arrays[0], arrays[2], arrays[7], arrays[9]
    return (
        ep_count == 16
        and tp_count == 2
        and query_weight.shape[0] % 128 == 0
        and past_keys.shape[2] == 2
        and break_offset.shape[1] == 4
        and past_keys.shape[3] == 128
        and past_keys.shape[1] % 128 == 0
        and tokens.shape[0] == 16
        and arrays[14].shape[0] == 1
        and arrays[12].shape[1] <= 64
    )


def fused_kernel(
    tokens_h, gains_v, wq_h, wk_h, wv_h, wo_h, keys_h, values_h, offset_h, lengths_h,
    router_h, routes_h, eg_h, eu_h, ed_h, sg_h, su_h, sd_h,
    mixed_o, fk_o, fv_o,
    tok, w_qkv, w_o, kc, vc, off, lens, rt, routes, e1, e2, s1, s2,
    nrm, tok_in, q_send, q_in, kv_send, kv_in, q4, tmat, oint, p4, ho,
    sc_in, f_send, f_in, f_in2, sq_send, sq_in, nf_in, resid, d_send, y_in, x_send, x_in, z_send, z_in, hilo, ones, sums,
    loc, core_s, core_r, tok_s, tok_r, qs, qr, kvs, kvr, scs, scr, fs, fr, gs, gr, sqs, sqr,
    nzs, nzr, nxs, nxr, ys, yr, xs, xr, zs, zr,
):
    e = lax.axis_index("ep")
    t = lax.axis_index("tp")
    c = lax.rem(e, 2)
    p = e // 2
    x = lax.rem(p, 2)
    z = p // 2
    seqs = tok.shape[0]
    width = tok.shape[1]
    pair = width // 8
    half = width // 2
    span = kc.shape[1]
    experts = router_h.shape[0]

    def ep_id(peer):
        return {"ep": peer * 2 + c}

    core_id = {"ep": p * 2 + (1 - c)}
    tp_id = {"tp": 1 - t}

    def remote(src, dst, ssem, rsem, device):
        return pltpu.make_async_remote_copy(
            src_ref=src, dst_ref=dst, send_sem=ssem, recv_sem=rsem,
            device_id=device, device_id_type=MESH,
        )

    barrier = pltpu.get_barrier_semaphore()
    for k in range(1, 8):
        pl.semaphore_signal(barrier, inc=1, device_id=ep_id(lax.rem(p + k, 8)), device_id_type=MESH)
    pl.semaphore_signal(barrier, inc=1, device_id=core_id, device_id_type=MESH)
    pl.semaphore_signal(barrier, inc=1, device_id=tp_id, device_id_type=MESH)

    qc, kcs = wq_h.shape[1], wk_h.shape[1]
    eff = eg_h.shape[2]
    early = [
        (tokens_h, tok),
        (wq_h, w_qkv.at[c, :, pl.ds(0, qc)]),
        (wk_h, w_qkv.at[c, :, pl.ds(qc, kcs)]),
        (wv_h, w_qkv.at[c, :, pl.ds(qc + kcs, kcs)]),
        (offset_h, off),
        (lengths_h, lens),
        (routes_h, routes),
        (router_h, rt.at[0]),
        (router_h, rt.at[1]),
        (wo_h, w_o.at[c]),
        (keys_h, kc),
        (values_h, vc),
        (sg_h, s1.at[:, pl.ds(0, eff)]),
        (su_h, s1.at[:, pl.ds(eff, eff)]),
        (sd_h, s2),
        (eg_h.at[0], e1.at[c, :, pl.ds(0, eff)]),
        (eu_h.at[0], e1.at[c, :, pl.ds(eff, eff)]),
        (ed_h.at[0], e2.at[c]),
    ]
    local = [pltpu.make_async_copy(a, b, loc.at[i]) for i, (a, b) in enumerate(early)]
    for copy in local:
        copy.start()

    local[0].wait()
    data = tok[...].astype(F32)
    factor = lax.rsqrt(jnp.mean(data * data, axis=-1, keepdims=True) + epsilon)
    normed = (data * factor * gains_v[:, 0:width]).astype(BF16)
    for k in range(8):
        nrm[k] = normed[:, k * pair : (k + 1) * pair]

    pl.semaphore_wait(barrier, 9)

    def spread(src_at, dst, ssem, rsem):
        out = []
        for k in range(1, 8):
            peer = lax.rem(p + k, 8)
            out.append(remote(src_at(peer), dst.at[p], ssem.at[k], rsem.at[k], ep_id(peer)))
        return out

    def landing(src, dst, ssem, rsem):
        out = []
        for k in range(1, 8):
            out.append(remote(src, dst.at[lax.rem(p - k + 8, 8)], ssem.at[k], rsem.at[k], ep_id(lax.rem(p + k, 8))))
        return out

    tok_copies = spread(lambda peer: nrm.at[peer], tok_in, tok_s, tok_r)
    for copy in tok_copies:
        copy.start()
    pieces = [
        (wq_h, w_qkv.at[c, :, pl.ds(0, qc)], w_qkv.at[1 - c, :, pl.ds(0, qc)]),
        (wk_h, w_qkv.at[c, :, pl.ds(qc, kcs)], w_qkv.at[1 - c, :, pl.ds(qc, kcs)]),
        (wv_h, w_qkv.at[c, :, pl.ds(qc + kcs, kcs)], w_qkv.at[1 - c, :, pl.ds(qc + kcs, kcs)]),
        (wo_h, w_o.at[c], w_o.at[1 - c]),
        (eg_h.at[0], e1.at[c, :, pl.ds(0, eff)], e1.at[1 - c, :, pl.ds(0, eff)]),
        (eu_h.at[0], e1.at[c, :, pl.ds(eff, eff)], e1.at[1 - c, :, pl.ds(eff, eff)]),
        (ed_h.at[0], e2.at[c], e2.at[1 - c]),
    ]
    core_out = [remote(a, b, core_s.at[i], core_r.at[i], core_id) for i, (a, b, _) in enumerate(pieces)]
    core_in = [remote(a, d, core_s.at[i], core_r.at[i], core_id) for i, (a, _, d) in enumerate(pieces)]
    for copy in core_out:
        copy.start()
    tok_in[p] = nrm[p]

    ri = lax.broadcasted_iota(jnp.int32, (256, 256), 0)
    ci = lax.broadcasted_iota(jnp.int32, (256, 256), 1)
    perm = (ci == 2 * lax.rem(ri, 128) + ri // 128).astype(F32).astype(BF16)
    same = lax.rem(ri, 2) == lax.rem(ci, 2)
    ones[:, 0:256] = jnp.where(same & (ri > ci), 1.0, 0.0).astype(BF16)
    ones[:, 256:512] = jnp.where(same, 1.0, 0.0).astype(BF16)

    def split(values):
        high = values.astype(BF16)
        return high, (values - high.astype(F32)).astype(BF16)

    local[4].wait()
    local[5].wait()
    for m in range(span // 256):
        cols = pl.ds(m * 128, 128)
        left = jnp.concatenate([off[:, 0, cols], off[:, 1, cols]], axis=0)
        right = jnp.concatenate([off[:, 2, cols], off[:, 3, cols]], axis=0)
        high, low = split(jnp.concatenate([left, right], axis=1))
        oint[:, m * 256 : (m + 1) * 256] = jnp.dot(high, perm, preferred_element_type=F32) + jnp.dot(
            low, perm, preferred_element_type=F32
        )
    rows2 = 2 * seqs
    lane_id = lax.broadcasted_iota(jnp.int32, (rows2, seqs), 1)
    row_id = lax.rem(lax.broadcasted_iota(jnp.int32, (rows2, seqs), 0), seqs)
    limit = jnp.sum(
        jnp.where(lane_id == row_id, jnp.broadcast_to(lens[...].astype(F32), (rows2, seqs)), 0.0),
        axis=1, keepdims=True,
    )

    for i in (1, 2, 3):
        local[i].wait()
    for i in range(3):
        core_in[i].wait_recv()
    for copy in landing(nrm.at[0], tok_in, tok_s, tok_r):
        copy.wait_recv()
    feats = tok_in[...].reshape(8 * seqs, pair)
    qw = w_qkv[:, :, 0:qc].reshape(pair, qc)
    q_send[...] = jnp.dot(feats, qw, preferred_element_type=F32).astype(BF16).reshape(8, seqs, qc)
    q_copies = spread(lambda peer: q_send.at[peer], q_in, qs, qr)
    for copy in q_copies:
        copy.start()
    q_in[p] = q_send[p]
    kvw = w_qkv[:, :, qc:].reshape(pair, 2 * kcs)
    kv_send[...] = jnp.dot(feats, kvw, preferred_element_type=F32).astype(BF16).reshape(8, seqs, 2 * kcs)
    kv_in[p] = kv_send[p]
    local[10].wait()
    local[11].wait()
    for copy in landing(q_send.at[0], q_in, qs, qr):
        copy.wait_recv()
    kv_copies = spread(lambda peer: kv_send.at[peer], kv_in, kvs, kvr)
    for copy in kv_copies:
        copy.start()

    queries = jnp.sum(q_in[...].astype(F32), axis=0)
    for r in range(4):
        q4[:, r, :] = queries[:, r * 128 : (r + 1) * 128]
    even_row = lax.rem(lax.broadcasted_iota(jnp.int32, (1, span), 1), 2) == 0

    def score(b, _):
        s = lax.dot_general(
            q4[b].astype(BF16), kc[b], (((1,), (1,)), ((), ())), preferred_element_type=F32
        )
        tmat[pl.ds(b, 1), :] = jnp.where(even_row, s[0:1], s[2:3])
        tmat[pl.ds(seqs + b, 1), :] = jnp.where(even_row, s[1:2], s[3:4])
        return 0

    lax.fori_loop(0, seqs, score, 0, unroll=2)

    blocks = span // 256
    scale = 128.0 ** (-0.5)
    lane = lax.broadcasted_iota(jnp.int32, (rows2, 256), 1)
    even = lax.rem(lane, 2) == 0
    place = (lane // 2).astype(F32)
    for m in range(blocks):
        cols = slice(m * 256, (m + 1) * 256)
        part = slice(m * rows2, (m + 1) * rows2)
        logits = tmat[:, cols] * scale + oint[:, cols]
        log_sig = jnp.minimum(logits, 0.0) - jnp.log(1.0 + jnp.exp(-jnp.abs(logits)))
        keep = jnp.where(place < limit - (m * 128), log_sig - logits, 0.0)
        high, low = split(keep)
        tmat[:, cols] = log_sig
        hilo[0, part] = high
        hilo[1, part] = low
    sums[...] = jnp.dot(
        hilo[...].reshape(2 * blocks * rows2, 256), ones[...], preferred_element_type=F32
    ).reshape(2, blocks * rows2, 512)
    carry = jnp.zeros((rows2, 256), F32)
    for m in range(blocks - 1, -1, -1):
        cols = slice(m * 256, (m + 1) * 256)
        part = slice(m * rows2, (m + 1) * rows2)
        after = carry + (sums[0, part, 0:256] + sums[1, part, 0:256])
        carry = carry + (sums[0, part, 256:512] + sums[1, part, 256:512])
        sticks = jnp.where(place < limit - (m * 128), jnp.exp(tmat[:, cols] + after), 0.0)
        on_even = jnp.where(even, sticks, 0.0)
        on_odd = jnp.where(even, 0.0, sticks)
        p4[:, 0, cols] = on_even[0:seqs]
        p4[:, 1, cols] = on_even[seqs:]
        p4[:, 2, cols] = on_odd[0:seqs]
        p4[:, 3, cols] = on_odd[seqs:]

    def weigh(b, _):
        ho[b] = jnp.dot(p4[b].astype(BF16), vc[b], preferred_element_type=F32)
        return 0

    lax.fori_loop(0, seqs, weigh, 0, unroll=2)
    heads = jnp.concatenate([ho[:, r, :] for r in range(4)], axis=1)
    scaled = (heads * gains_v[:, 2 * width : 2 * width + qc]).astype(BF16)
    sc_in[p] = scaled
    square = jnp.broadcast_to(jnp.sum(heads * heads, axis=-1, keepdims=True), (seqs, 128))
    sq_send[...] = square
    sc_copies = spread(lambda peer: sc_in.at[p], sc_in, scs, scr)
    for copy in sc_copies:
        copy.start()
    sq_copy = remote(sq_send, sq_in, sqs.at[0], sqr.at[0], tp_id)
    sq_copy.start()

    local[9].wait()
    core_in[3].wait_recv()
    for copy in landing(sc_in.at[p], sc_in, scs, scr):
        copy.wait_recv()
    f_send[...] = lax.dot_general(
        sc_in[...].reshape(8 * seqs, qc), w_o[...].reshape(pair, qc), (((1,), (1,)), ((), ())),
        preferred_element_type=F32,
    ).astype(BF16).reshape(8, seqs, pair)
    f_copies = spread(lambda peer: f_send.at[peer], f_in, fs, fr)
    for copy in f_copies:
        copy.start()
    f_in[p] = f_send[p]
    g_copies = [remote(f_in.at[p], f_in2.at[p], gs.at[0], gr.at[0], tp_id)]
    g_copies[0].start()
    f_land = landing(f_send.at[0], f_in, fs, fr)
    for k in range(1, 8):
        f_land[k - 1].wait_recv()
        slot = lax.rem(p - k + 8, 8)
        copy = remote(f_in.at[slot], f_in2.at[slot], gs.at[k], gr.at[k], tp_id)
        copy.start()
        g_copies.append(copy)
    sq_copy.wait_recv()
    for copy in g_copies:
        copy.wait_recv()
    total = sq_send[:, 0:1] + sq_in[:, 0:1]
    norm = lax.rsqrt(total / (HQ * HD) + epsilon)
    attention = jnp.concatenate([f_in[k].astype(F32) + f_in2[k].astype(F32) for k in range(8)], axis=1) * norm
    residual = (tok[...].astype(F32) + attention).astype(BF16).astype(F32)
    resid[0] = residual[:, 0:half]
    resid[1] = residual[:, half:]
    factor = lax.rsqrt(jnp.mean(residual * residual, axis=-1, keepdims=True) + epsilon)
    nf = (residual * factor * gains_v[:, width : 2 * width]).astype(BF16)

    for i in (6, 7, 8):
        local[i].wait()
    router = jnp.concatenate([rt[0], rt[1]], axis=0)
    pads = 128 - 2 * experts
    router = jnp.concatenate([router, jnp.zeros((pads, width), BF16)], axis=0)
    prob = jax.nn.sigmoid(
        lax.dot_general(nf, router, (((1,), (1,)), ((), ())), preferred_element_type=F32)
    )
    sub = lax.broadcasted_iota(jnp.int32, (128, seqs), 0)
    sub = jnp.where(sub < 2 * experts, lax.rem(sub, experts), -1)
    named = jnp.zeros((128, seqs), F32)
    for k in range(routes.shape[0]):
        named = named + jnp.where(sub == routes[k : k + 1, :], 1.0, 0.0)
    eye = jnp.where(
        lax.broadcasted_iota(jnp.int32, (seqs, seqs), 0) == lax.broadcasted_iota(jnp.int32, (seqs, seqs), 1), 1.0, 0.0
    ).astype(BF16)
    hot = lax.dot_general(eye, named.astype(BF16), (((1,), (1,)), ((), ())), preferred_element_type=F32)
    picked = hot * prob
    lanes = lax.broadcasted_iota(jnp.int32, (seqs, 128), 1)
    bottom = jnp.sum(jnp.where(lanes < experts, picked, 0.0), axis=-1, keepdims=True)
    share = routed_scale * picked / bottom
    high, low = split(share)
    nf_in[p, :, 0:width] = nf
    nf_in[p, :, width : width + 128] = jnp.where(lanes < experts, high.astype(F32), low.astype(F32)).astype(BF16)

    xp = z * 2 + (1 - x)
    nx_copies = [remote(nf_in.at[p], nf_in.at[p], nxs.at[0], nxr.at[0], ep_id(xp))]
    nz_copies = []
    for k in range(1, 4):
        peer = lax.rem(z + k, 4) * 2 + x
        nz_copies.append(remote(nf_in.at[p], nf_in.at[p], nzs.at[k], nzr.at[k], ep_id(peer)))
    for copy in nz_copies:
        copy.start()
    nx_copies[0].start()

    for i in (12, 13, 14):
        local[i].wait()
    gu = jnp.dot(nf, s1[...], preferred_element_type=F32)
    hidden = (jax.nn.silu(gu[:, 0:eff]) * gu[:, eff:]).astype(BF16)
    shared = jnp.dot(hidden, s2[...], preferred_element_type=F32)

    for k in range(1, 4):
        slot = lax.rem(z - k + 4, 4) * 2 + x
        remote(nf_in.at[p], nf_in.at[slot], nzs.at[k], nzr.at[k], ep_id(p)).wait_recv()
        copy = remote(nf_in.at[slot], nf_in.at[slot], nxs.at[k], nxr.at[k], ep_id(xp))
        copy.start()
        nx_copies.append(copy)
    for i in (15, 16, 17):
        local[i].wait()
    for i in (4, 5, 6):
        core_in[i].wait_recv()
    for k in range(4):
        slot = lax.rem(z - k + 4, 4) * 2 + (1 - x)
        remote(nf_in.at[p], nf_in.at[slot], nxs.at[k], nxr.at[k], ep_id(xp)).wait_recv()

    everyone = nf_in[:, :, 0:width].reshape(8 * seqs, width)
    shares = nf_in[:, :, width : width + 128].reshape(8 * seqs, 128).astype(F32)
    big_lane = lax.broadcasted_iota(jnp.int32, (8 * seqs, 128), 1)
    routed = []
    for j in range(2):
        mine = 2 * p + j
        col = jnp.sum(
            jnp.where((big_lane == mine) | (big_lane == experts + mine), shares, 0.0), axis=-1, keepdims=True
        )
        gu = jnp.dot(everyone, e1[j], preferred_element_type=F32)
        routed.append((jax.nn.silu(gu[:, 0:eff]) * gu[:, eff:] * col).astype(BF16))
    acts = jnp.concatenate(routed, axis=1)
    for g in range(4):
        cols = slice(g * (width // 4), (g + 1) * (width // 4))
        part = jnp.dot(acts, e2[:, :, cols].reshape(2 * eff, width // 4), preferred_element_type=F32)
        inner = slice((g % 2) * (half // 2), (g % 2 + 1) * (half // 2))
        d_send[g // 2, :, :, inner] = part.astype(BF16).reshape(8, seqs, width // 4)
    d_send[0, p] = (d_send[0, p].astype(F32) + shared[:, 0:half]).astype(BF16)
    d_send[1, p] = (d_send[1, p].astype(F32) + shared[:, half:]).astype(BF16)

    y_copies = {}
    for side in (1, 0):
        for k in (1, 2, 3, 0):
            xx = lax.rem(x + side, 2)
            slot = lax.rem(z + k, 4) * 2 + xx
            yslot = lax.rem(z + k, 4) * 2 + xx
            copy = remote(d_send.at[1 - t, slot], y_in.at[yslot], ys.at[4 * side + k], yr.at[4 * side + k], tp_id)
            copy.start()
            y_copies[side, k] = copy
    x_copies = {}
    for k in (1, 2, 3, 0):
        slot = lax.rem(z + k, 4) * 2 + (1 - x)
        y_copies[1, k].wait_recv()
        x_send[k] = (d_send[t, slot].astype(F32) + y_in[slot].astype(F32)).astype(BF16)
        copy = remote(x_send.at[k], x_in.at[k], xs.at[k], xr.at[k], ep_id(xp))
        copy.start()
        x_copies[k] = copy
    z_copies = {}
    for k in (1, 2, 3, 0):
        zz = lax.rem(z + k, 4)
        slot = zz * 2 + x
        y_copies[0, k].wait_recv()
        x_copies[k].wait_recv()
        summed = d_send[t, slot].astype(F32) + y_in[slot].astype(F32) + x_in[k].astype(F32)
        if k > 0:
            z_send[k - 1] = summed.astype(BF16)
            copy = remote(z_send.at[k - 1], z_in.at[k - 1], zs.at[k], zr.at[k], ep_id(slot))
            copy.start()
            z_copies[k] = copy
    for copy in landing(kv_send.at[0], kv_in, kvs, kvr):
        copy.wait_recv()
    fresh = jnp.sum(kv_in[...].astype(F32), axis=0)
    fk_o[...] = fresh[:, 0:kcs].astype(BF16)
    fv_o[...] = fresh[:, kcs:].astype(BF16)
    for k in range(1, 4):
        z_copies[k].wait_recv()
        summed = summed + z_in[k - 1].astype(F32)
    mixed_o[...] = (resid[t] + summed).astype(BF16)

    for copy in (
        tok_copies + core_out + q_copies + kv_copies + sc_copies + [sq_copy] + f_copies + g_copies
        + nz_copies + nx_copies + list(y_copies.values()) + list(x_copies.values()) + list(z_copies.values())
    ):
        copy.wait_send()


def fused_body(
    ep_count, tp_count, tokens, attn_gain, query_weight, key_weight, value_weight, out_weight, head_gain,
    past_keys, past_values, break_offset, cache_lengths, ffn_gain, router_weight, expert_routes,
    expert_gate, expert_up, expert_down, shared_gate, shared_up, shared_down,
):
    seqs, width = tokens.shape
    pair = width // 8
    half = width // 2
    rows, qc = query_weight.shape
    kcs = key_weight.shape[1]
    positions = past_keys.shape[1]
    span = 2 * positions
    eff = expert_gate.shape[2]
    experts = router_weight.shape[1]
    tops = expert_routes.shape[1]
    gains = jnp.concatenate([attn_gain, ffn_gain, head_gain]).astype(F32)[None, :]
    operands = (
        tokens, gains, query_weight, key_weight, value_weight, out_weight,
        past_keys.reshape(seqs, span, HD), past_values.reshape(seqs, span, HD),
        break_offset, cache_lengths.reshape(1, seqs), router_weight.T, expert_routes.T,
        expert_gate, expert_up, expert_down, shared_gate, shared_up, shared_down,
    )
    anywhere = pl.BlockSpec(memory_space=pl.ANY)
    inside = pl.BlockSpec(memory_space=pltpu.VMEM)
    vm = pltpu.VMEM
    dma = pltpu.SemaphoreType.DMA
    scratch = [
        vm((seqs, width), BF16), vm((2, rows, qc + 2 * kcs), BF16), vm((2, rows, qc), BF16),
        vm((seqs, span, HD), BF16), vm((seqs, span, HD), BF16), vm(break_offset.shape, F32),
        vm((1, seqs), jnp.int32), vm((2, experts, width), BF16), vm((tops, seqs), jnp.int32),
        vm((2, width, 2 * eff), BF16), vm((2, eff, width), BF16), vm((width, 2 * eff), BF16), vm((eff, width), BF16),
        vm((8, seqs, pair), BF16), vm((8, seqs, pair), BF16),
        vm((8, seqs, qc), BF16), vm((8, seqs, qc), BF16), vm((8, seqs, 2 * kcs), BF16), vm((8, seqs, 2 * kcs), BF16),
        vm((seqs, 4, HD), F32), vm((2 * seqs, span), F32), vm((2 * seqs, span), F32), vm((seqs, 4, span), F32),
        vm((seqs, 4, HD), F32),
        vm((8, seqs, qc), BF16), vm((8, seqs, pair), BF16), vm((8, seqs, pair), BF16), vm((8, seqs, pair), BF16),
        vm((seqs, 128), F32), vm((seqs, 128), F32), vm((8, seqs, width + 128), BF16), vm((2, seqs, half), F32),
        vm((2, 8, seqs, half), BF16), vm((8, seqs, half), BF16), vm((4, seqs, half), BF16), vm((4, seqs, half), BF16),
        vm((3, seqs, half), BF16), vm((3, seqs, half), BF16),
        vm((2, span // 256 * 2 * seqs, 256), BF16), vm((256, 512), BF16), vm((2, span // 256 * 2 * seqs, 512), F32),
        dma((18,)), dma((7,)), dma((7,)),
        dma((8,)), dma((8,)), dma((8,)), dma((8,)), dma((8,)), dma((8,)), dma((8,)), dma((8,)),
        dma((8,)), dma((8,)), dma((8,)), dma((8,)), dma((1,)), dma((1,)),
        dma((4,)), dma((4,)), dma((4,)), dma((4,)), dma((8,)), dma((8,)), dma((4,)), dma((4,)), dma((4,)), dma((4,)),
    ]
    return pl.pallas_call(
        fused_kernel,
        out_shape=(
            jax.ShapeDtypeStruct((seqs, half), BF16),
            jax.ShapeDtypeStruct((seqs, kcs), BF16),
            jax.ShapeDtypeStruct((seqs, kcs), BF16),
        ),
        in_specs=[inside if i == 1 else anywhere for i in range(len(operands))],
        out_specs=(inside, inside, inside),
        scratch_shapes=scratch,
        compiler_params=pltpu.CompilerParams(
            collective_id=0, has_side_effects=True, vmem_limit_bytes=60 * 1024 * 1024
        ),
    )(*operands)


def solution(mesh):
    placed = (
        P("ep", None),
        P(),
        P("ep", "tp"),
        P("ep", "tp"),
        P("ep", "tp"),
        P("ep", "tp"),
        P("tp"),
        P("ep", None, "tp", None),
        P("ep", None, "tp", None),
        P("ep", "tp", None),
        P("ep"),
        P(),
        P(),
        P("ep", None),
        P("ep", None, "tp"),
        P("ep", None, "tp"),
        P("ep", "tp", None),
        P(None, "tp"),
        P(None, "tp"),
        P("tp", None),
    )
    ep_count, tp_count = mesh.shape["ep"], mesh.shape["tp"]

    def chosen_body(*arrays):
        if fits(ep_count, tp_count, arrays):
            return fused_body(ep_count, tp_count, *arrays)
        return body(*arrays)

    return jax.shard_map(
        chosen_body,
        mesh=mesh,
        in_specs=placed,
        out_specs=(P("ep", "tp"), P("ep", "tp"), P("ep", "tp")),
        check_vma=False,
    )
```
